512 devices in a mesh: sp: 16 (over y, x), tp: 32 (over z, core).
Axes of the slice: x: 4, y: 4, z: 16, core: 2. Of those that a mesh axis runs over, the one named last changes fastest.
Arguments:
- tokens: bfloat16 [32, 2048, 4096], P('tp', 'sp'), may hold values from -6 to 6
- latent_down_matrix: bfloat16 [4096, 512], P('tp'), may hold values from -0.09375 to 0.09375
- rope_weight: bfloat16 [4096, 64], P('tp'), may hold values from -0.09375 to 0.09375
- latent_norm_scale: float32 [512], replicated, may hold values from 0.1 to 1.9
- key_up_matrix: bfloat16 [512, 32, 128], P(None, 'tp'), may hold values from -0.25 to 0.25
- value_up_matrix: bfloat16 [512, 32, 128], P(None, 'tp'), may hold values from -0.25 to 0.25
- query: bfloat16 [32, 32, 192], P('sp', 'tp'), may hold values from -126 to 126
Outputs:
- plain_key_cache: bfloat16 [32, 2048, 32, 128], P('sp', None, 'tp')
- head_value_cache: bfloat16 [32, 2048, 32, 128], P('sp', None, 'tp')
- rotated_key_cache: bfloat16 [32, 2048, 64], P('sp')
- first_read: bfloat16 [32, 32, 128], P('sp', 'tp')
The draws below stay inside these ranges and needn't reach their ends.
All inputs are finite; a program needn't handle non-finite values.
Results may differ from the reference program's by a relative error of at most 0.035.
Values may be sent and summed in bfloat16 or wider, within the bound.
No kernel may reach another device: no remote copies, remote signals or barrier semaphores. Data moves between devices by JAX's collectives and lax.ppermute only.
A program may use at most 64 MiB of HBM per device.

```python
import jax
import jax.numpy as jnp
from jax import lax

MODEL_WIDTH = 4096
LATENT_WIDTH = 512
ROPE = 64
PLAIN_KEY_WIDTH = 128
VALUE_WIDTH = 128
ATTENTION_HEADS = 32
SEQUENCE_COUNT = 32
SEQUENCE_LENGTH = 2048


def draw_query(key, part):
    base = jnp.clip(jax.random.normal(jax.random.fold_in(key, 11), (SEQUENCE_COUNT, ATTENTION_HEADS, PLAIN_KEY_WIDTH + ROPE), jnp.float32), -3.5, 3.5) * 3.0
    return base.astype(jnp.bfloat16)


def block_scale(key, dims, split, least, top_value):
    level = 1.0
    for dim, parts in split:
        heights = jax.random.uniform(jax.random.fold_in(jax.random.fold_in(key, 6), dim), (parts,), jnp.float32, least / len(split), top_value / len(split))
        level = level * jnp.repeat(jnp.exp(heights), dims[dim] // parts).reshape((-1,) + (1,) * (len(dims) - 1 - dim))
    return level


def gaussian(rng, shape, scale, most, cuts=(), kind=jnp.bfloat16):
    factor_of = block_scale(rng, shape, cuts, -0.22, 0.18) if cuts else 1.0
    array = jax.random.normal(rng, shape, jnp.float32) * scale * factor_of
    return jnp.minimum(jnp.maximum(array, -most), most).astype(kind)


def setup_inputs(seed: int = 0) -> dict:
    key_list = jax.random.split(jax.random.key(seed), 8)
    return {
        "tokens": gaussian(key_list[0], (SEQUENCE_COUNT, SEQUENCE_LENGTH, MODEL_WIDTH), 1.0, 6.0, ((0, 32), (1, 16))),
        "latent_down_matrix": gaussian(key_list[1], (MODEL_WIDTH, LATENT_WIDTH), MODEL_WIDTH ** -0.5, 0.09375, ((0, 32),)),
        "rope_weight": gaussian(key_list[2], (MODEL_WIDTH, ROPE), MODEL_WIDTH ** -0.5, 0.09375, ((0, 32),)),
        "latent_norm_scale": jnp.clip(1.0 + 0.18 * jax.random.normal(key_list[3], (LATENT_WIDTH,), jnp.float32), 0.1, 1.9),
        "key_up_matrix": gaussian(key_list[4], (LATENT_WIDTH, ATTENTION_HEADS, PLAIN_KEY_WIDTH), LATENT_WIDTH ** -0.5, 0.25, ((1, 32),)),
        "value_up_matrix": gaussian(key_list[5], (LATENT_WIDTH, ATTENTION_HEADS, VALUE_WIDTH), LATENT_WIDTH ** -0.5, 0.25, ((1, 32),)),
        "query": draw_query(jax.random.fold_in(key_list[7], 71), 0),
    }


def rotate(part, positions):
    half = part.shape[-1] // 2
    freqs = 1.0 / 10000.0 ** (jnp.arange(half, dtype=jnp.float32) * 2.0 / part.shape[-1])
    angles = positions.astype(jnp.float32)[:, None] * freqs
    cosine = jnp.cos(angles)
    sine = jnp.sin(angles)
    first = part[..., :half]
    second = part[..., half:]
    return jnp.concatenate([first * cosine - second * sine, second * cosine + first * sine], axis=-1)

def reference(tokens, latent_down_matrix, rope_weight, latent_norm_scale, key_up_matrix, value_up_matrix, query):
    flat = tokens.reshape(SEQUENCE_COUNT * SEQUENCE_LENGTH, MODEL_WIDTH)
    latent = jnp.dot(flat, latent_down_matrix, preferred_element_type=jnp.float32)
    scaled = latent * lax.rsqrt(lax.optimization_barrier(jnp.mean(latent * latent, axis=-1, keepdims=True)) + 1e-06)
    latent_normalized = (scaled * latent_norm_scale.astype(jnp.float32)).astype(jnp.bfloat16)
    rope = jnp.dot(flat, rope_weight, preferred_element_type=jnp.float32).reshape(SEQUENCE_COUNT, SEQUENCE_LENGTH, ROPE)
    positions = jnp.arange(SEQUENCE_LENGTH, dtype=jnp.int32)
    rotated_key_cache = rotate(rope, positions).astype(jnp.bfloat16)
    plain_key_cache = jnp.dot(latent_normalized, key_up_matrix.reshape(LATENT_WIDTH, ATTENTION_HEADS * PLAIN_KEY_WIDTH), preferred_element_type=jnp.float32).astype(jnp.bfloat16).reshape(SEQUENCE_COUNT, SEQUENCE_LENGTH, ATTENTION_HEADS, PLAIN_KEY_WIDTH)
    head_value_cache = jnp.dot(latent_normalized, value_up_matrix.reshape(LATENT_WIDTH, ATTENTION_HEADS * VALUE_WIDTH), preferred_element_type=jnp.float32).astype(jnp.bfloat16).reshape(SEQUENCE_COUNT, SEQUENCE_LENGTH, ATTENTION_HEADS, VALUE_WIDTH)
    query_float = query.astype(jnp.float32)
    query_plain = query[..., :PLAIN_KEY_WIDTH]
    rotated_query = rotate(query_float[..., PLAIN_KEY_WIDTH:], jnp.full((1,), SEQUENCE_LENGTH, jnp.int32)).astype(jnp.bfloat16)
    factor = 1.0 / (PLAIN_KEY_WIDTH + ROPE) ** 0.5

    def attend(items):
        plain, turned, keys, values, rotary = items
        scores = jnp.einsum('hd,lhd->hl', plain.astype(jnp.float32), keys.astype(jnp.float32))
        scores = scores + jnp.einsum('hd,ld->hl', turned.astype(jnp.float32), rotary.astype(jnp.float32))
        scores = scores * factor
        weights = jnp.exp(scores - lax.optimization_barrier(jnp.max(scores, axis=-1, keepdims=True)))
        total = lax.optimization_barrier(jnp.sum(weights, axis=-1, keepdims=True))
        rounded = weights.astype(jnp.bfloat16)
        mixed = jnp.einsum('hl,lhd->hd', rounded.astype(jnp.float32), values.astype(jnp.float32))
        return (mixed / total).astype(jnp.bfloat16)
    first_read = lax.map(attend, (query_plain, rotated_query, plain_key_cache, head_value_cache, rotated_key_cache))
    return (plain_key_cache, head_value_cache, rotated_key_cache, first_read)
```

```python
import jax
import jax.numpy as jnp
import numpy as np
from jax import lax
from jax.experimental import pallas as pl
from jax.experimental.pallas import tpu as pltpu
from jax.sharding import PartitionSpec as P

PLACE = (
    (7, 3, 0, 12, 8, 11, 2, 6, 4, 15, 1, 10, 13, 5, 14, 9),
    (1, 10, 15, 6, 2, 4, 8, 12, 11, 0, 7, 3, 9, 14, 5, 13),
    (4, 15, 10, 14, 9, 1, 13, 5, 7, 3, 11, 0, 2, 6, 12, 8),
    (6, 2, 9, 1, 10, 14, 3, 7, 5, 13, 12, 8, 15, 4, 11, 0),
    (10, 1, 4, 2, 6, 15, 12, 8, 0, 11, 3, 7, 14, 9, 13, 5),
    (11, 0, 3, 5, 13, 7, 9, 14, 1, 10, 4, 15, 8, 12, 6, 2),
    (2, 6, 14, 10, 1, 9, 7, 3, 13, 5, 8, 12, 4, 15, 0, 11),
    (8, 12, 5, 3, 7, 13, 1, 10, 9, 14, 2, 6, 11, 0, 15, 4),
    (13, 5, 12, 0, 11, 8, 4, 15, 2, 6, 9, 14, 7, 3, 10, 1),
    (9, 14, 6, 15, 4, 2, 11, 0, 8, 12, 13, 5, 1, 10, 3, 7),
    (0, 11, 7, 13, 5, 3, 14, 9, 10, 1, 15, 4, 12, 8, 2, 6),
    (3, 7, 11, 8, 12, 0, 6, 2, 15, 4, 10, 1, 5, 13, 9, 14),
    (5, 13, 8, 11, 0, 12, 15, 4, 6, 2, 14, 9, 3, 7, 1, 10),
    (12, 8, 13, 7, 3, 5, 10, 1, 14, 9, 6, 2, 0, 11, 4, 15),
    (15, 4, 1, 9, 14, 10, 5, 13, 3, 7, 0, 11, 6, 2, 8, 12),
    (14, 9, 2, 4, 15, 6, 0, 11, 12, 8, 5, 13, 10, 1, 7, 3),
)

W_SCALE = 2.0**19
LAT_SCALE = 2.0**10
ROPE_SCALE = 2.0**4
VMEM = pl.BlockSpec(memory_space=pltpu.VMEM)
SMEM = pl.BlockSpec(memory_space=pltpu.SMEM)


def down_kernel(tab, tok, mine, other, gain, cos, sin, out):
    width = mine.shape[2]
    rows = tok.shape[0]
    lat = jnp.zeros((rows, width), jnp.float32)
    rope = jnp.zeros((rows, 64), jnp.float32)
    for half, w in enumerate((mine, other)):
        for j in range(0, 16, 2):
            x = jnp.concatenate(
                [
                    tok[:, pl.ds(pl.multiple_of(tab[16 * half + i], 128), 128)]
                    for i in (j, j + 1)
                ],
                axis=1,
            )
            lat += jnp.dot(
                x, w[j : j + 2, :128, :].reshape(256, width), preferred_element_type=jnp.float32
            )
            wr = jnp.concatenate(
                [
                    jnp.concatenate(
                        [w[i, 128:144, k * 128 : (k + 1) * 128] for k in range(4)], axis=0
                    )
                    for i in (j, j + 1)
                ],
                axis=1,
            )
            rope += lax.dot_general(
                x, wr, (((1,), (1,)), ((), ())), preferred_element_type=jnp.float32
            )
    lat = lat * (1.0 / W_SCALE)
    scaled = lat * lax.rsqrt(jnp.mean(lat * lat, axis=-1, keepdims=True) + 1e-06)
    out[0:128, :] = (scaled * gain[...]).astype(jnp.bfloat16)
    turned = jnp.transpose(rope * (1.0 / W_SCALE))
    first, second = turned[:32], turned[32:]
    c, s = cos[...], sin[...]
    a = (first * c - second * s).astype(jnp.bfloat16)
    b = (second * c + first * s).astype(jnp.bfloat16)
    out[128:144, :] = jnp.concatenate([a[:16], a[16:], b[:16], b[16:]], axis=1)


def up_kernel(tab, mine, other, wk, wv, qp, qt, keys, values, rot, read):
    wkv = jnp.concatenate([wk[...], wv[...]], axis=1)
    for half, y in enumerate((mine, other)):
        s = tab[16] if half == 0 else 1 - tab[16]
        for p in range(16):
            x = y[tab[p]]
            kv = jnp.dot(x[:128], wkv, preferred_element_type=jnp.float32).astype(jnp.bfloat16)
            keys[s, p * 128 : (p + 1) * 128, :] = kv[:, :128]
            values[s, p * 128 : (p + 1) * 128, :] = kv[:, 128:]
            for k in range(4):
                rot[s, k * 16 : (k + 1) * 16, p * 128 : (p + 1) * 128] = x[
                    128:144, k * 128 : (k + 1) * 128
                ]
        scores = lax.dot_general(
            qp[s], keys[s], (((1,), (1,)), ((), ())), preferred_element_type=jnp.float32
        )
        scores = scores + jnp.dot(qt[s], rot[s], preferred_element_type=jnp.float32)
        scores = scores * (1.0 / 192.0**0.5)
        weights = jnp.exp(scores - jnp.max(scores, axis=-1, keepdims=True))
        total = jnp.sum(weights, axis=-1, keepdims=True)
        mixed = jnp.dot(
            weights.astype(jnp.bfloat16), values[s], preferred_element_type=jnp.float32
        )
        read[s] = (mixed / total).astype(jnp.bfloat16)


def turn(positions, half):
    freqs = 1.0 / 10000.0 ** (jnp.arange(half, dtype=jnp.float32) / half)
    angles = freqs[:, None] * positions.astype(jnp.float32)[None, :]
    return jnp.cos(angles), jnp.sin(angles)


def body(tokens, down, rope_w, gain, key_up, value_up, query):
    place = np.array(PLACE)
    origin = np.zeros((16, 16), np.int32)
    for p in range(16):
        for q in range(16):
            origin[place[p][q]][p] = q
    col = lax.axis_index("sp")
    tp = lax.axis_index("tp")
    z, core = tp // 2, tp % 2
    both = ("sp", "tp")
    lines = [[2 * k + c for k in range(16)] for c in range(2)]
    swap = [(t, t ^ 1) for t in range(32)]

    packed = jnp.concatenate(
        [
            down,
            jnp.concatenate([rope_w.T[16 * k : 16 * (k + 1)] for k in range(4)], axis=1),
        ],
        axis=0,
    )
    packed = (packed.astype(jnp.float32) * W_SCALE).astype(jnp.float16)
    along = [
        (p * 32 + 2 * q + c, p * 32 + 2 * int(place[p][q]) + c)
        for p in range(16)
        for q in range(16)
        for c in range(2)
    ]
    moved = lax.ppermute(packed, both, along)
    mine = lax.all_gather(moved, "sp", axis=0).astype(jnp.bfloat16)
    other = lax.ppermute(mine, "tp", swap)

    chips = jnp.asarray(origin)[z]
    tab = jnp.concatenate([chips * 256 + core * 128, chips * 256 + (1 - core) * 128]).astype(
        jnp.int32
    )
    cos, sin = turn(col * 128 + jnp.arange(128, dtype=jnp.int32), 32)
    block = pl.pallas_call(
        down_kernel,
        out_shape=jax.ShapeDtypeStruct((144, 512), jnp.bfloat16),
        in_specs=[SMEM, VMEM, VMEM, VMEM, VMEM, VMEM, VMEM],
        out_specs=VMEM,
        cost_estimate=pl.CostEstimate(
            flops=2 * 128 * 4096 * 576, bytes_accessed=6 << 20, transcendentals=0
        ),
    )(tab, tokens[0], mine, other, gain.reshape(1, 512), cos, sin)

    level = jnp.concatenate(
        [jnp.full((128, 1), LAT_SCALE, jnp.float32), jnp.full((16, 1), ROPE_SCALE, jnp.float32)]
    )
    block = (block.astype(jnp.float32) * level).astype(jnp.float16)
    across = [
        (p * 32 + 2 * q + c, q * 32 + 2 * int(place[p][q]) + c)
        for p in range(16)
        for q in range(16)
        for c in range(2)
    ]
    block = lax.ppermute(block, both, across)
    line = lax.all_gather(block, "tp", axis=0, axis_index_groups=lines)
    line = (line.astype(jnp.float32) * (1.0 / level)).astype(jnp.bfloat16)
    pair = lax.ppermute(line, "tp", swap)

    query_plain = query[..., :128]
    last = query[..., 128:].astype(jnp.float32)
    qc, qs = turn(jnp.full((1,), 2048, jnp.int32), 32)
    qc, qs = qc[:, 0], qs[:, 0]
    first, second = last[..., :32], last[..., 32:]
    query_turned = jnp.concatenate(
        [first * qc - second * qs, second * qc + first * qs], axis=-1
    ).astype(jnp.bfloat16)
    tab2 = jnp.concatenate([jnp.asarray(place.T)[col], core[None]]).astype(jnp.int32)
    keys, values, rot, read = pl.pallas_call(
        up_kernel,
        out_shape=(
            jax.ShapeDtypeStruct((2, 2048, 128), jnp.bfloat16),
            jax.ShapeDtypeStruct((2, 2048, 128), jnp.bfloat16),
            jax.ShapeDtypeStruct((2, 64, 2048), jnp.bfloat16),
            jax.ShapeDtypeStruct((2, 1, 128), jnp.bfloat16),
        ),
        in_specs=[SMEM] + [VMEM] * 6,
        out_specs=(VMEM,) * 4,
        cost_estimate=pl.CostEstimate(
            flops=2 * 4096 * 512 * 256, bytes_accessed=8 << 20, transcendentals=4096
        ),
    )(tab2, line, pair, key_up[:, 0], value_up[:, 0], query_plain, query_turned)
    return (
        keys[:, :, None, :],
        values[:, :, None, :],
        jnp.swapaxes(rot, 1, 2),
        read,
    )


def solution(mesh):
    in_specs = (
        P("tp", "sp", None),
        P("tp", None),
        P("tp", None),
        P(),
        P(None, "tp", None),
        P(None, "tp", None),
        P("sp", "tp", None),
    )
    out_specs = (
        P("sp", None, "tp", None),
        P("sp", None, "tp", None),
        P("sp", None, None),
        P("sp", "tp", None),
    )
    return jax.shard_map(body, mesh=mesh, in_specs=in_specs, out_specs=out_specs, check_vma=False)
```
